32 devices in a mesh: sp: 16 (over z, y, x), tp: 2 (over core).
Axes of the slice: x: 2, y: 2, z: 4, core: 2. Of those that a mesh axis runs over, the one named last changes fastest.
Arguments:
- stream: bfloat16 [4096, 2048], P(('sp', 'tp')), may hold values from -6 to 6
- outer_gate: bfloat16 [4096, 1024], P('sp', 'tp'), may hold values from -6 to 6
- inner_gate: bfloat16 [4096, 1024], P('sp', 'tp'), may hold values from -6 to 6
- conv_values: bfloat16 [4096, 1024], P('sp', 'tp'), may hold values from -6 to 6
- doc_ids: int32 [4096], P('sp'), may hold values from 0 to 7, never falling along the last dimension, each value on 1 to 1024 neighbouring positions
- conv_taps: float32 [3, 1024], P(None, 'tp'), may hold values from -3.5 to 3.5
- out_weight: bfloat16 [1024, 2048], replicated, may hold values from -0.1875 to 0.1875
- norm_gain: float32 [2048], replicated, may hold values from 0.1 to 1.9
- route_ids: int32 [4096, 2], P(('sp', 'tp')), may hold values from 0 to 31, all different within a row; in each aligned block of 128 rows (0 to 127, 128 to 255, ...) at most 16 rows name the same one
- route_logits: float32 [4096, 2], P(('sp', 'tp')), may hold values from -4 to 4
- group_weight: float32 [4096], P(('sp', 'tp')), may hold values from 0.25 to 1
- w_gate: bfloat16 [32, 2048, 1024], P(('sp', 'tp')), may hold values from -0.125 to 0.125
- w_up: bfloat16 [32, 2048, 1024], P(('sp', 'tp')), may hold values from -0.125 to 0.125
- w_down: bfloat16 [32, 1024, 2048], P(('sp', 'tp')), may hold values from -0.1875 to 0.1875
Outputs:
- result: bfloat16 [4096, 2048], P(('sp', 'tp'))
The draws below stay inside these ranges and needn't reach their ends.
Inputs may be any that keep to these rules, and one draw needn't show every extreme that they name: `route_ids`: the two experts of a token differ. In the rows of one device (aligned blocks of 128 rows) no expert is named more than 16 times, a bound that some block reaches. `doc_ids`: document numbers never fall along the sequence; a document has 1 to 1024 positions and one has exactly 1024.
All inputs are finite; a program needn't handle non-finite values.
Results may differ from the reference program's by a relative error of at most 0.0052.
Values may be sent and summed in bfloat16 or wider, within the bound.
No kernel may reach another device: no remote copies, remote signals or barrier semaphores. Data moves between devices by JAX's collectives and lax.ppermute only.
A program may use at most 64 MiB of HBM per device.

```python
import math
import jax
import jax.numpy as jnp
import numpy as np
from jax import lax

D = 2048
CW = 1024
FF = 1024
TOPK = 2
ROWS = 128
TOKENS = 4096
EXPERTS = 32
CAP = 16
DOCS = 8
MOST_DOC = 1024


def levels(key, shape, cuts, least, high):
    def one(axis_at, shards_of):
        steps = jax.random.uniform(jax.random.fold_in(jax.random.fold_in(key, 6), axis_at), (shards_of,), jnp.float32, least / len(cuts), high / len(cuts))
        return jnp.repeat(jnp.exp(steps), shape[axis_at] // shards_of).reshape((-1,) + (1,) * (len(shape) - axis_at - 1))

    level = one(*cuts[0])
    for cut in cuts[1:]:
        level = level * one(*cut)
    return level


def length_profile(number_of, total, limit, lean):
    portions = [(1 << 20) // math.isqrt(grade ** lean) + 1 for grade in range(2, number_of + 1)]
    surplus, given = total - limit - (number_of - 1), [1] * (number_of - 1)
    while surplus > 0:
        movable = [i for i in range(number_of - 1) if given[i] < limit]
        mass, budget = sum([portions[i] for i in movable]), surplus
        for i in movable:
            extra = min(limit - given[i], max(1, budget * portions[i] // mass), surplus)
            given[i] = given[i] + extra
            surplus = surplus - extra
    return np.array([limit] + given)


def ragged(stream_key, count, total, bound, lean):
    if count == 2:
        one = jax.random.randint(stream_key, (), max(1, total - bound), min(bound, total - 1) + 1)
        return jnp.stack([one, total - one])
    tallies = jnp.asarray(length_profile(count, total, bound, lean), jnp.int32)
    twos = (count - 1) // 2
    giver, taker = tallies[1:1 + 2 * twos:2], tallies[2:2 + 2 * twos:2]
    margin = jnp.minimum(giver - 1, bound - taker)
    passed = jax.random.randint(jax.random.fold_in(stream_key, 1), (twos,), 0, 1 << 20) % (margin + 1)
    tallies = tallies.at[1:1 + 2 * twos:2].set(giver - passed).at[2:2 + 2 * twos:2].set(taker + passed)
    return tallies[jax.random.permutation(jax.random.fold_in(stream_key, 2), count)]


def routed_block(rng, own, number, rows, amount, top, bound, slope):
    sequence = jax.random.permutation(rng, amount)
    packed, ordinary = portions_of(amount, rows * top, bound, slope, True), portions_of(amount, rows * top, bound, slope, False)
    places = jnp.arange(amount)

    def named(sizes, turn):
        used = int((sizes > 0).sum())
        fixed = max(1, used // 4)
        passed = fixed + (places - fixed + turn * (used - fixed)) % max(1, amount - fixed)
        return jnp.zeros((amount,), jnp.int32).at[sequence[jnp.where(places < fixed, places, passed)]].set(jnp.asarray(sizes, jnp.int32))

    sizes = jnp.where(number % 4 == 0, named(packed, number // 4), named(ordinary, number - number // 4 - 1))
    mixed = jax.random.permutation(jax.random.fold_in(own, 3), amount)
    donor, taker = mixed[0:amount // 2 * 2:2], mixed[1:amount // 2 * 2:2]
    slack = jnp.minimum(sizes[donor] - 1, bound - sizes[taker]) // 2
    slack = jnp.where((donor == sequence[0]) | (taker == sequence[0]) | (sizes[taker] == 0), 0, jnp.maximum(slack, 0))
    passed = jax.random.randint(jax.random.fold_in(own, 4), (amount // 2,), 0, 1 << 20) % (slack + 1)
    sizes = sizes.at[donor].add(-passed).at[taker].add(passed)
    members = jnp.searchsorted(jnp.cumsum(sizes), jnp.arange(rows * top), side="right").astype(jnp.int32)
    grid = members.reshape(top, rows).T
    grid = grid[jax.random.permutation(jax.random.fold_in(own, 1), rows)]
    turn = jax.random.randint(jax.random.fold_in(own, 2), (rows, 1), 0, top)
    return jnp.take_along_axis(grid, (jnp.arange(top)[None, :] + turn) % top, axis=1)


def portions_of(count, total, bound, lean, full):
    loads = [(1 << 20) // math.isqrt(rank ** lean) + 1 for rank in range(1, count + 1)]
    largest = bound if full else min(bound, max(-(-total // count), total * loads[0] // sum(loads)))
    least = 1 if total - largest >= count - 1 else 0
    counts, surplus = [largest] + [least] * (count - 1), total - largest - least * (count - 1)
    while surplus > 0:
        candidates = [i for i in range(1, count) if counts[i] < largest] or [i for i in range(1, count) if counts[i] < bound]
        mass, remaining = sum([loads[i] for i in candidates]), surplus
        for i in candidates:
            extra = min(bound - counts[i], max(1, remaining * loads[i] // mass), surplus)
            counts[i] = counts[i] + extra
            surplus = surplus - extra
    return np.array(counts)


def noise(stream_key, dims, deviation, bound, pieces=(), held_as=jnp.bfloat16):
    result = jax.random.normal(stream_key, dims, jnp.float32) * deviation
    if len(pieces) > 0:
        result = levels(stream_key, dims, pieces, -0.22, 0.18) * result
    return jnp.clip(result, min=-bound, max=bound).astype(held_as)


def setup_inputs(seed: int = 0) -> dict:
    arg_keys = jax.random.split(jax.random.key(seed), 15)
    stream = noise(arg_keys[0], (TOKENS, D), 1.0, 6.0, ((0, 32),))
    outer_gate = noise(arg_keys[1], (TOKENS, CW), 1.0, 6.0, ((0, 16), (1, 2)))
    inner_gate = noise(arg_keys[2], (TOKENS, CW), 1.0, 6.0, ((0, 16), (1, 2)))
    conv_values = noise(arg_keys[3], (TOKENS, CW), 1.0, 6.0, ((0, 16), (1, 2)))
    doc_ids = jnp.searchsorted(jnp.cumsum(ragged(arg_keys[4], DOCS, TOKENS, MOST_DOC, 1)), jnp.arange(TOKENS), side="right").astype(jnp.int32)
    conv_taps = noise(arg_keys[5], (3, CW), 3 ** -0.5, 3.5, ((1, 2),), jnp.float32)
    out_weight = noise(arg_keys[6], (CW, D), CW ** -0.5, 0.1875)
    norm_gain = jnp.clip(1.0 + 0.18 * jax.random.normal(arg_keys[7], (D,), jnp.float32), 0.1, 1.9)
    route_ids_keys = jax.random.split(jax.random.fold_in(arg_keys[8], 1), TOKENS // ROWS)
    route_ids_turns = jax.random.permutation(jax.random.fold_in(arg_keys[8], 3), TOKENS // ROWS)
    route_ids = jax.vmap(lambda own, number: routed_block(jax.random.fold_in(arg_keys[8], 2), own, number, ROWS, EXPERTS, TOPK, CAP, 2))(route_ids_keys, route_ids_turns).reshape((TOKENS, TOPK))
    route_logits = noise(arg_keys[9], (TOKENS, TOPK), 1.5, 4.0, ((0, 32),), jnp.float32)
    group_weight = jnp.clip(jnp.exp(math.log(1.0) - 1.3862944 * jax.random.uniform(arg_keys[10], (TOKENS,), jnp.float32) ** levels(arg_keys[10], (TOKENS,), ((0, 32),), -0.2, 0.2)), 0.25, 1.0)
    w_gate = noise(arg_keys[11], (EXPERTS, D, FF), D ** -0.5, 0.125, ((0, 32),))
    w_up = noise(arg_keys[12], (EXPERTS, D, FF), D ** -0.5, 0.125, ((0, 32),))
    w_down = noise(arg_keys[13], (EXPERTS, FF, D), FF ** -0.5, 0.1875, ((0, 32),))
    return {"stream": stream, "outer_gate": outer_gate, "inner_gate": inner_gate, "conv_values": conv_values, "doc_ids": doc_ids, "conv_taps": conv_taps, "out_weight": out_weight, "norm_gain": norm_gain, "route_ids": route_ids, "route_logits": route_logits, "group_weight": group_weight, "w_gate": w_gate, "w_up": w_up, "w_down": w_down}


def reference(stream, outer_gate, inner_gate, conv_values, doc_ids, conv_taps, out_weight, norm_gain, route_ids, route_logits, group_weight, w_gate, w_up, w_down):
    product = (inner_gate.astype(jnp.float32) * conv_values.astype(jnp.float32)).astype(jnp.bfloat16)
    prod_f = product.astype(jnp.float32)
    padded = jnp.pad(prod_f, ((1, 1), (0, 0)))
    padded_docs = jnp.pad(doc_ids, (1, 1), constant_values=-1)
    same_prev = (padded_docs[:-2] == doc_ids).astype(jnp.float32)[:, None]
    same_next = (padded_docs[2:] == doc_ids).astype(jnp.float32)[:, None]
    conv = conv_taps[0] * padded[:-2] * same_prev + conv_taps[1] * prod_f + conv_taps[2] * padded[2:] * same_next
    mixed = (outer_gate.astype(jnp.float32) * conv).astype(jnp.bfloat16)
    resid = stream.astype(jnp.float32) + jnp.dot(mixed, out_weight, preferred_element_type=jnp.float32)
    scale = lax.rsqrt(lax.optimization_barrier(jnp.mean(resid * resid, axis=-1, keepdims=True)) + 1e-06)
    normed = (resid * scale * norm_gain).astype(jnp.bfloat16)
    expo = jnp.exp(route_logits)
    gate = group_weight[:, None] * expo / lax.optimization_barrier(jnp.sum(expo, axis=1, keepdims=True))
    flat_ids = route_ids.reshape(-1)
    gate_flat = gate.reshape(-1)
    load = EXPERTS * CAP
    count_all = flat_ids.shape[0]

    def step(total, expert):
        is_hit = flat_ids == expert
        rank = jnp.cumsum(is_hit.astype(jnp.int32)) - 1
        where_to = jnp.where(is_hit, rank, load).astype(jnp.int32)
        pick = jnp.zeros((load,), jnp.int32).at[where_to].set(jnp.arange(count_all, dtype=jnp.int32), mode='drop')
        is_live = jnp.zeros((load,), gate_flat.dtype).at[where_to].set(1.0, mode='drop')
        token_of = pick // TOPK
        rows_in = normed[token_of]
        hidden = (jax.nn.silu(jnp.dot(rows_in, w_gate[expert], preferred_element_type=jnp.float32)) * jnp.dot(rows_in, w_up[expert], preferred_element_type=jnp.float32)).astype(jnp.bfloat16)
        expert_out = jnp.dot(hidden, w_down[expert], preferred_element_type=jnp.float32).astype(jnp.bfloat16)
        weights = gate_flat[pick] * is_live
        total = total.at[token_of].add(expert_out.astype(jnp.float32) * weights[:, None])
        return (total, None)
    total, unused = lax.scan(step, resid, jnp.arange(EXPERTS, dtype=jnp.int32))
    return total.astype(jnp.bfloat16)
```

```python
import jax
import jax.numpy as jnp
from jax import lax
from jax.sharding import PartitionSpec as P

CHUNKS = 1


def on_device(
    stream,
    outer_gate,
    inner_gate,
    conv_values,
    doc_ids,
    conv_taps,
    out_weight,
    norm_gain,
    route_ids,
    route_logits,
    group_weight,
    w_gate,
    w_up,
    w_down,
):
    f32, bf16 = jnp.float32, jnp.bfloat16
    tok_rows, width = stream.shape
    channels_here = inner_gate.shape[1]

    def gated(rows):
        return (inner_gate[rows].astype(f32) * conv_values[rows].astype(f32)).astype(bf16)

    sp = lax.axis_size("sp")
    up = [(i, (i + 1) % sp) for i in range(sp - 1)]
    down = [(j, i) for i, j in up]
    lanes = 128

    def edge(rows):
        doc = jnp.broadcast_to(doc_ids[rows].astype(bf16)[:, None], (1, lanes))
        return jnp.concatenate([gated(rows), doc], axis=1)

    before = lax.ppermute(edge(slice(-1, None)), "sp", up)
    after = lax.ppermute(edge(slice(0, 1)), "sp", down)

    expert_total = lax.axis_size("sp") * lax.axis_size("tp")
    top_count = route_ids.shape[1]
    capacity = 2 * tok_rows * top_count // expert_total
    slot_count = expert_total * capacity
    names = jnp.arange(expert_total, dtype=jnp.int32)
    hits = [route_ids[:, k][:, None] == names[None, :] for k in range(top_count)]
    named = sum(h.astype(bf16) for h in hits)
    row_at = lax.broadcasted_iota(jnp.int32, (tok_rows, tok_rows), 0)
    col_at = lax.broadcasted_iota(jnp.int32, (tok_rows, tok_rows), 1)
    earlier = jnp.dot((col_at < row_at).astype(bf16), named, preferred_element_type=f32)
    rank = jnp.stack([jnp.sum(jnp.where(h, earlier, 0.0), axis=1) for h in hits]).astype(jnp.int32)
    ids = jnp.stack([route_ids[:, k] for k in range(top_count)])
    part = capacity // CHUNKS
    slot = (rank // part) * (expert_total * part) + ids * part + rank % part
    expo = jnp.exp(route_logits)
    gate = group_weight[:, None] * expo / jnp.sum(expo, axis=1, keepdims=True)

    product = gated(slice(None))
    prod = product.astype(f32)
    doc_before = before[:, channels_here].astype(jnp.int32)
    doc_after = after[:, channels_here].astype(jnp.int32)
    docs_prev = jnp.concatenate([doc_before, doc_ids[:-1]])
    docs_next = jnp.concatenate([doc_ids[1:], doc_after])
    same_prev = (docs_prev == doc_ids).astype(f32)[:, None]
    same_next = (docs_next == doc_ids).astype(f32)[:, None]
    prod_prev = jnp.concatenate([before[:, :channels_here], product[:-1]], axis=0).astype(f32)
    prod_next = jnp.concatenate([product[1:], after[:, :channels_here]], axis=0).astype(f32)
    conv = (
        conv_taps[0] * prod_prev * same_prev
        + conv_taps[1] * prod
        + conv_taps[2] * prod_next * same_next
    )
    mixed = (outer_gate.astype(f32) * conv).astype(bf16)
    halves = lax.all_to_all(
        mixed.reshape(-1, tok_rows, channels_here), "tp", split_axis=0, concat_axis=0, tiled=True
    )
    weights = out_weight.reshape(-1, channels_here, width)
    resid = stream.astype(f32)
    for i in range(weights.shape[0]):
        resid = resid + jnp.dot(halves[i], weights[i], preferred_element_type=f32)
    scale = lax.rsqrt(jnp.mean(resid * resid, axis=-1, keepdims=True) + 1e-06)
    normed = (resid * scale * norm_gain).astype(bf16)

    chunk_slots = expert_total * part
    result = resid
    arrived = []
    for c in range(CHUNKS):
        at = c * chunk_slots + lax.broadcasted_iota(jnp.int32, (chunk_slots, tok_rows), 0)
        pick = sum((at == slot[k][None, :]).astype(bf16) for k in range(top_count))
        outgoing = jnp.dot(pick, normed, preferred_element_type=f32).astype(bf16)
        arrived.append(
            lax.all_to_all(
                outgoing.reshape(expert_total, part, width),
                ("sp", "tp"), split_axis=0, concat_axis=0, tiled=True,
            )
        )
    returned = []
    for c in range(CHUNKS):
        rows_in = arrived[c].reshape(chunk_slots, width)
        hidden = (
            jax.nn.silu(jnp.dot(rows_in, w_gate[0], preferred_element_type=f32))
            * jnp.dot(rows_in, w_up[0], preferred_element_type=f32)
        ).astype(bf16)
        outputs = jnp.dot(hidden, w_down[0], preferred_element_type=f32).astype(bf16)
        returned.append(
            lax.all_to_all(
                outputs.reshape(expert_total, part, width),
                ("sp", "tp"), split_axis=0, concat_axis=0, tiled=True,
            )
        )
    for c in range(CHUNKS):
        at = c * chunk_slots + lax.broadcasted_iota(jnp.int32, (tok_rows, chunk_slots), 1)
        spread = sum(
            jnp.where(at == slot[k][:, None], gate[:, k][:, None], 0.0) for k in range(top_count)
        )
        high = lax.reduce_precision(spread, 8, 7)
        both = jnp.concatenate([high.astype(bf16), (spread - high).astype(bf16)], axis=0)
        added = jnp.dot(both, returned[c].reshape(chunk_slots, width), preferred_element_type=f32)
        result = result + (added[:tok_rows] + added[tok_rows:])
    return result.astype(bf16)


def solution(mesh):
    placed = (
        P(("sp", "tp"), None),
        P("sp", "tp"),
        P("sp", "tp"),
        P("sp", "tp"),
        P("sp"),
        P(None, "tp"),
        P(),
        P(),
        P(("sp", "tp"), None),
        P(("sp", "tp"), None),
        P(("sp", "tp")),
        P(("sp", "tp"), None, None),
        P(("sp", "tp"), None, None),
        P(("sp", "tp"), None, None),
    )
    return jax.shard_map(
        on_device, mesh=mesh, in_specs=placed, out_specs=P(("sp", "tp"), None), check_vma=False
    )
```

```python
import jax
import jax.numpy as jnp
from jax import lax
from jax.experimental import pallas as pl
from jax.experimental.pallas import tpu as pltpu
from jax.sharding import PartitionSpec as P

CHUNKS = 1
LANES = 128


def edge_rows(inner_gate, conv_values, doc_ids):
    rows, chans = inner_gate.shape
    tile = 16
    last = rows // tile - 1

    def body(doc, in_first, in_last, val_first, val_last, first, final):
        for out, a, b, at, row in (
            (first, in_first, val_first, 0, 0),
            (final, in_last, val_last, rows - 1, tile - 1),
        ):
            product = a[...].astype(jnp.float32) * b[...].astype(jnp.float32)
            out[:, :chans] = product[row : row + 1].astype(jnp.bfloat16)
            number = doc[at].astype(jnp.float32)
            out[:, chans:] = jnp.full((1, LANES), number, jnp.float32).astype(jnp.bfloat16)

    head = pl.BlockSpec((tile, chans), lambda i: (0, 0))
    tail = pl.BlockSpec((tile, chans), lambda i: (last, 0))
    whole = pl.BlockSpec((1, chans + LANES), lambda i: (0, 0))
    row = jax.ShapeDtypeStruct((1, chans + LANES), jnp.bfloat16)
    return pl.pallas_call(
        body,
        grid=(1,),
        in_specs=[pl.BlockSpec(memory_space=pltpu.SMEM), head, tail, head, tail],
        out_specs=[whole, whole],
        out_shape=[row, row],
    )(doc_ids, inner_gate, inner_gate, conv_values, conv_values)


def masked_conv(inner_gate, conv_values, outer_gate, doc_ids, conv_taps, before, after):
    rows, chans = inner_gate.shape
    f32 = jnp.float32

    def body(inner, values, outer, docs, taps, prev_edge, next_edge, out):
        product = (inner[...].astype(f32) * values[...].astype(f32)).astype(jnp.bfloat16)
        product = product.astype(f32)
        row_at = lax.broadcasted_iota(jnp.int32, (rows, rows), 0)
        col_at = lax.broadcasted_iota(jnp.int32, (rows, rows), 1)
        doc_row = docs[...].astype(f32)

        def column(offset):
            kept = jnp.where(col_at == row_at + offset, doc_row, 0.0)
            return jnp.sum(kept, axis=1, keepdims=True)

        at = lax.broadcasted_iota(jnp.int32, (rows, 1), 0)
        own = column(0)
        prev_doc = jnp.where(at == 0, prev_edge[:, chans : chans + 1].astype(f32), column(-1))
        next_doc = jnp.where(at == rows - 1, next_edge[:, chans : chans + 1].astype(f32), column(1))
        same_prev = (prev_doc == own).astype(f32)
        same_next = (next_doc == own).astype(f32)
        prod_prev = jnp.where(at == 0, prev_edge[:, :chans].astype(f32), pltpu.roll(product, 1, 0))
        prod_next = jnp.where(
            at == rows - 1, next_edge[:, :chans].astype(f32), pltpu.roll(product, rows - 1, 0)
        )
        conv = (
            taps[0:1] * prod_prev * same_prev
            + taps[1:2] * product
            + taps[2:3] * prod_next * same_next
        )
        out[...] = (outer[...].astype(f32) * conv).astype(jnp.bfloat16)

    return pl.pallas_call(
        body, out_shape=jax.ShapeDtypeStruct((rows, chans), jnp.bfloat16)
    )(inner_gate, conv_values, outer_gate, doc_ids.reshape(1, rows), conv_taps, before, after)


def expert_mlp(rows_in, w_gate, w_up, w_down):
    count, width = rows_in.shape
    inner = w_gate.shape[1]
    first, second = 4, 4
    f_block, d_block = inner // first, width // second
    f32 = jnp.float32

    def body(x, gate, up, down, out, hidden):
        for f in range(first):
            here = slice(f * f_block, (f + 1) * f_block)
            g = jnp.dot(x[...], gate[:, here], preferred_element_type=f32)
            u = jnp.dot(x[...], up[:, here], preferred_element_type=f32)
            hidden[:, here] = (g / (1.0 + jnp.exp(-g)) * u).astype(jnp.bfloat16)
        for d in range(second):
            here = slice(d * d_block, (d + 1) * d_block)
            out[:, here] = jnp.dot(
                hidden[...], down[:, here], preferred_element_type=f32
            ).astype(out.dtype)

    vmem = pl.BlockSpec(memory_space=pltpu.VMEM)
    return pl.pallas_call(
        body,
        in_specs=[vmem, vmem, vmem, vmem],
        out_specs=vmem,
        out_shape=jax.ShapeDtypeStruct((count, width), jnp.bfloat16),
        scratch_shapes=[pltpu.VMEM((count, inner), jnp.bfloat16)],
        compiler_params=pltpu.CompilerParams(vmem_limit_bytes=32 << 20),
    )(rows_in, w_gate, w_up, w_down)


def on_device(
    stream,
    outer_gate,
    inner_gate,
    conv_values,
    doc_ids,
    conv_taps,
    out_weight,
    norm_gain,
    route_ids,
    route_logits,
    group_weight,
    w_gate,
    w_up,
    w_down,
):
    f32, bf16 = jnp.float32, jnp.bfloat16
    tok_rows, width = stream.shape
    channels_here = inner_gate.shape[1]

    sp = lax.axis_size("sp")
    up = [(i, (i + 1) % sp) for i in range(sp - 1)]
    down = [(j, i) for i, j in up]
    leading, last = edge_rows(inner_gate, conv_values, doc_ids)
    before = lax.ppermute(last, "sp", up)
    after = lax.ppermute(leading, "sp", down)

    expert_total = lax.axis_size("sp") * lax.axis_size("tp")
    top_count = route_ids.shape[1]
    capacity = 2 * tok_rows * top_count // expert_total
    slot_count = expert_total * capacity
    names = jnp.arange(expert_total, dtype=jnp.int32)
    hits = [route_ids[:, k][:, None] == names[None, :] for k in range(top_count)]
    named = sum(h.astype(bf16) for h in hits)
    row_at = lax.broadcasted_iota(jnp.int32, (tok_rows, tok_rows), 0)
    col_at = lax.broadcasted_iota(jnp.int32, (tok_rows, tok_rows), 1)
    earlier = jnp.dot((col_at < row_at).astype(bf16), named, preferred_element_type=f32)
    rank = jnp.stack([jnp.sum(jnp.where(h, earlier, 0.0), axis=1) for h in hits]).astype(jnp.int32)
    ids = jnp.stack([route_ids[:, k] for k in range(top_count)])
    part = capacity // CHUNKS
    slot = (rank // part) * (expert_total * part) + ids * part + rank % part
    expo = jnp.exp(route_logits)
    gate = group_weight[:, None] * expo / jnp.sum(expo, axis=1, keepdims=True)

    mixed = masked_conv(
        inner_gate, conv_values, outer_gate, doc_ids, conv_taps, before, after
    )
    halves = lax.all_to_all(
        mixed.reshape(-1, tok_rows, channels_here), "tp", split_axis=0, concat_axis=0, tiled=True
    )
    weights = out_weight.reshape(-1, channels_here, width)
    resid = stream.astype(f32)
    for i in range(weights.shape[0]):
        resid = resid + jnp.dot(halves[i], weights[i], preferred_element_type=f32)
    scale = lax.rsqrt(jnp.mean(resid * resid, axis=-1, keepdims=True) + 1e-06)
    normed = (resid * scale * norm_gain).astype(bf16)

    chunk_slots = expert_total * part
    result = resid
    arrived = []
    for c in range(CHUNKS):
        at = c * chunk_slots + lax.broadcasted_iota(jnp.int32, (chunk_slots, tok_rows), 0)
        pick = sum((at == slot[k][None, :]).astype(bf16) for k in range(top_count))
        outgoing = jnp.dot(pick, normed, preferred_element_type=f32).astype(bf16)
        arrived.append(
            lax.all_to_all(
                outgoing.reshape(expert_total, part, width),
                ("sp", "tp"), split_axis=0, concat_axis=0, tiled=True,
            )
        )
    returned = []
    for c in range(CHUNKS):
        rows_in = arrived[c].reshape(chunk_slots, width)
        outputs = expert_mlp(rows_in, w_gate[0], w_up[0], w_down[0])
        returned.append(
            lax.all_to_all(
                outputs.reshape(expert_total, part, width),
                ("sp", "tp"), split_axis=0, concat_axis=0, tiled=True,
            )
        )
    for c in range(CHUNKS):
        at = c * chunk_slots + lax.broadcasted_iota(jnp.int32, (tok_rows, chunk_slots), 1)
        spread = sum(
            jnp.where(at == slot[k][:, None], gate[:, k][:, None], 0.0) for k in range(top_count)
        )
        high = lax.reduce_precision(spread, 8, 7)
        both = jnp.concatenate([high.astype(bf16), (spread - high).astype(bf16)], axis=0)
        added = jnp.dot(both, returned[c].reshape(chunk_slots, width), preferred_element_type=f32)
        result = result + (added[:tok_rows] + added[tok_rows:])
    return result.astype(bf16)


def solution(mesh):
    placed = (
        P(("sp", "tp"), None),
        P("sp", "tp"),
        P("sp", "tp"),
        P("sp", "tp"),
        P("sp"),
        P(None, "tp"),
        P(),
        P(),
        P(("sp", "tp"), None),
        P(("sp", "tp"), None),
        P(("sp", "tp")),
        P(("sp", "tp"), None, None),
        P(("sp", "tp"), None, None),
        P(("sp", "tp"), None, None),
    )
    return jax.shard_map(
        on_device, mesh=mesh, in_specs=placed, out_specs=P(("sp", "tp"), None), check_vma=False
    )
```
